512 devices in a mesh: sp: 32 (over z, x), dp: 16 (over y, core).
Axes of the slice: x: 4, y: 8, z: 8, core: 2. Of those that a mesh axis runs over, the one named last changes fastest.
Arguments:
- queries: bfloat16 [64, 8, 2048, 256], P('dp', None, 'sp'), may hold values from -6 to 6
- keys: bfloat16 [64, 8, 2048, 256], P('dp', None, 'sp'), may hold values from -6 to 6
- values: bfloat16 [64, 8, 2048, 256], P('dp', None, 'sp'), may hold values from -6 to 6
- log_decay: float32 [512, 2048], P(('dp', 'sp')), may hold values from -2 to 0, as said below
- w_out: bfloat16 [8, 256, 2048], P(None, None, 'dp'), may hold values from -0.125 to 0.125
Outputs:
- mixed_out: bfloat16 [64, 2048, 2048], P('dp', 'sp')
The draws below stay inside these ranges and needn't reach their ends.
Inputs may be any that keep to these rules, and one draw needn't show every extreme that they name: Every entry of log_decay is below zero.
All inputs are finite; a program needn't handle non-finite values.
Results may differ from the reference program's by a relative error of at most 0.008.
Values may be sent and summed in bfloat16 or wider, within the bound.
A program may use at most 128 MiB of HBM per device.

```python
import jax
import jax.numpy as jnp
from jax import lax

WIDTH = 2048
HEADS = 8
HEAD_DIM = 256
BLOCK = 64
SEG_DEV = 64
SEQUENCE_LENGTH = 2048
SEQUENCE_TOTAL = 64


def draw_log_decay(key, part):
    random_subkeys = jax.random.split(key, 7)
    order = jax.random.permutation(random_subkeys[0], HEADS)
    fast_count = HEADS // 2
    is_fast = order < fast_count
    fast_rate = jax.random.uniform(random_subkeys[1], (HEADS,), jnp.float32, 1.0 / 60.0, 1.0 / 30.0)
    slow_rate = jax.random.uniform(random_subkeys[2], (HEADS,), jnp.float32, 0.1, 0.5) / SEQUENCE_LENGTH
    per_head_rate = jnp.where(is_fast, fast_rate, slow_rate)
    segment_count = SEQUENCE_LENGTH // SEG_DEV
    segment_factor = jnp.exp(jax.random.uniform(random_subkeys[3], (SEQUENCE_TOTAL, segment_count), jnp.float32, jnp.log(0.5), jnp.log(2.0)))
    segment_factor = jnp.repeat(segment_factor, SEG_DEV, axis=1)
    coarse_estimate = jax.random.uniform(random_subkeys[4], (SEQUENCE_TOTAL, HEADS, SEQUENCE_LENGTH), jnp.float32, 0.6, 1.4)
    spike_position = jax.random.randint(random_subkeys[5], (SEQUENCE_TOTAL, 2), 0, SEQUENCE_LENGTH)
    spike_depth = jnp.log(jax.random.uniform(random_subkeys[6], (SEQUENCE_TOTAL, 2), jnp.float32, 0.6, 0.8))
    position_index = jnp.arange(SEQUENCE_LENGTH, dtype=jnp.int32)
    decay_spike = jnp.sum(jnp.where(position_index[None, None, :] == spike_position[:, :, None], spike_depth[:, :, None], 0.0), axis=1)
    final_output = -per_head_rate[None, :, None] * segment_factor[:, None, :] * coarse_estimate + decay_spike[:, None, :]
    return final_output.reshape(SEQUENCE_TOTAL * HEADS, SEQUENCE_LENGTH).astype(jnp.float32)


def steps_of(own_key, dims, pieces, least, largest):
    loudness, own = 1.0, jax.random.fold_in(own_key, 6)
    for axis_at, parts in pieces:
        draws = jnp.exp(jax.random.uniform(jax.random.fold_in(own, axis_at), (parts,), jnp.float32, least / len(pieces), largest / len(pieces)))
        loudness = loudness * jnp.repeat(draws, dims[axis_at] // parts).reshape([-1 if axis == axis_at else 1 for axis in range(len(dims))])
    return loudness


def centred(own_key, dims, scale, bound, shards=(), kind=jnp.bfloat16):
    entries = scale * jax.random.normal(own_key, dims, jnp.float32)
    if shards:
        entries = entries * steps_of(own_key, dims, shards, -0.22, 0.18)
    return jnp.clip(entries, -bound, bound).astype(kind)


def setup_inputs(seed: int = 0) -> dict:
    arg_keys = jax.random.split(jax.random.key(seed), 6)
    queries = centred(arg_keys[0], (SEQUENCE_TOTAL, HEADS, SEQUENCE_LENGTH, HEAD_DIM), 1.0, 6.0, ((0, 16), (2, 32)))
    keys = centred(arg_keys[1], (SEQUENCE_TOTAL, HEADS, SEQUENCE_LENGTH, HEAD_DIM), 1.0, 6.0, ((0, 16), (2, 32)))
    values = centred(arg_keys[2], (SEQUENCE_TOTAL, HEADS, SEQUENCE_LENGTH, HEAD_DIM), 1.0, 6.0, ((0, 16), (2, 32)))
    log_decay = draw_log_decay(jax.random.fold_in(arg_keys[5], 71), 0)
    w_out = centred(arg_keys[4], (HEADS, HEAD_DIM, WIDTH), (HEADS * HEAD_DIM) ** -0.5, 0.125, ((2, 16),))
    return dict(queries=queries, keys=keys, values=values, log_decay=log_decay, w_out=w_out)


def rotate(field_in, cosine, sine_tab):
    half_dim = field_in.shape[1] // 2
    widened = field_in.astype(jnp.float32)
    first_half = widened[:, :half_dim]
    second_half = widened[:, half_dim:]
    turned = jnp.concatenate([first_half * cosine - second_half * sine_tab, second_half * cosine + first_half * sine_tab], axis=1)
    return turned.astype(jnp.bfloat16)

def product(form, left_op, right_op):
    return jnp.einsum(form, left_op.astype(jnp.float32), right_op.astype(jnp.float32), precision=lax.Precision.HIGHEST)

def retain(query_rows, key_rows, value_rows, decay_row, cosine, sine_tab):
    length, head_width = query_rows.shape
    blocks = length // BLOCK
    rot_query = rotate(query_rows, cosine, sine_tab).reshape(blocks, BLOCK, head_width)
    rot_key = rotate(key_rows, cosine, sine_tab).reshape(blocks, BLOCK, head_width)
    value_blocks = value_rows.reshape(blocks, BLOCK, head_width)
    within = jnp.cumsum(decay_row.astype(jnp.float32).reshape(blocks, BLOCK), axis=1)
    ending = within[:, -1:]
    causal = jnp.tril(jnp.ones((BLOCK, BLOCK), dtype=bool))[None]
    spread = within[:, :, None] - within[:, None, :]
    decay_mask = jnp.where(causal, jnp.exp(jnp.where(causal, spread, 0.0)), 0.0)
    scores = product('bnd,bmd->bnm', rot_query, rot_key)
    weights = (scores * decay_mask).astype(jnp.bfloat16)
    scaled_keys = (rot_key.astype(jnp.float32) * jnp.exp(ending - within)[:, :, None]).astype(jnp.bfloat16)
    updates = product('bmd,bme->bde', scaled_keys, value_blocks)

    def advance(state_now, inputs):
        factor, update = inputs
        return (factor * state_now + update, state_now.astype(jnp.bfloat16))
    start_state = jnp.zeros((head_width, head_width), jnp.float32)
    _, before = lax.scan(advance, start_state, (jnp.exp(ending[:, 0]), updates))
    local_part = product('bnm,bme->bne', weights, value_blocks)
    carried = product('bnd,bde->bne', rot_query, before)
    combined = local_part + jnp.exp(within)[:, :, None] * carried
    return combined.reshape(length, head_width).astype(jnp.bfloat16)

def reference(queries, keys, values, log_decay, w_out):
    seq_count, head_count, length, head_width = queries.shape
    item_count = seq_count * head_count
    half_dim = head_width // 2
    frequency = 10000.0 ** (-jnp.arange(half_dim, dtype=jnp.float32) / half_dim)
    angles = jnp.arange(length, dtype=jnp.float32)[:, None] * frequency[None, :]
    cosine = jnp.cos(angles)
    sine_tab = jnp.sin(angles)

    def one_item(inputs):
        return retain(inputs[0], inputs[1], inputs[2], inputs[3], cosine, sine_tab)
    retained = lax.map(one_item, (queries.reshape(item_count, length, head_width), keys.reshape(item_count, length, head_width), values.reshape(item_count, length, head_width), log_decay))
    retained = retained.reshape(seq_count, head_count, length, head_width)

    def project(seq_rows):
        widened = seq_rows.astype(jnp.float32)
        normed = (widened * lax.rsqrt(lax.optimization_barrier(jnp.mean(widened * widened, axis=-1, keepdims=True)) + 1e-06)).astype(jnp.bfloat16)
        return product('htd,hde->te', normed, w_out).astype(jnp.bfloat16)
    return lax.map(project, retained)
```

```python
import functools

import jax
import jax.numpy as jnp
import numpy as np
from jax import lax
from jax.experimental import pallas as pl
from jax.experimental.pallas import tpu as pltpu
from jax.sharding import PartitionSpec as P

RING_X = 4
LANES = 128
MESH = pl.DeviceIdType.MESH
F32 = jnp.float32
BF16 = jnp.bfloat16


def take(ref, sem):
    pltpu.make_async_copy(ref, ref, sem).wait()


def kernel(
    dims,
    q_hbm, k_hbm, v_hbm, ld_hbm, w_hbm, freq_ref,
    out_ref,
    kv, qb, ldb, cosb, sinb, wrow, wcol, upd, s_in, s_out, o_snd, o_rcv, wb, acc,
    loc_w, ld_s, ld_r, kv_s, kv_r, q_s, q_r, ch_s, ch_r, o_s, o_r,
    wr_s, wr_r, wl_s, wl_r, p_s, p_r,
):
    X, Z, Y, G, J, T, D = dims
    N, L, HD = G * J, X * T, X * J * D
    R = Y // 2
    HALF = HD // 2
    sp, dp = lax.axis_index("sp"), lax.axis_index("dp")
    z, x = sp // X, sp % X
    y, c = dp // 2, dp % 2

    def at_x(d):
        return z * X + (x + d) % X

    def dp_of(yy):
        return ((yy + 2 * Y) % Y) * 2 + c

    right, left = dp_of(y + 1), dp_of(y - 1)
    mate = y * 2 + (1 - c)

    barrier = pltpu.get_barrier_semaphore()
    for d in range(1, X):
        pl.semaphore_signal(barrier, inc=1, device_id={"sp": at_x(d)}, device_id_type=MESH)
    for d in range(1, Z):
        pl.semaphore_signal(
            barrier, inc=1, device_id={"sp": ((z + d) % Z) * X + x}, device_id_type=MESH
        )
    for t in (right, left, mate):
        pl.semaphore_signal(barrier, inc=1, device_id={"dp": t}, device_id_type=MESH)
    pl.semaphore_wait(barrier, X + Z + 1)

    def remote(src, dst, ss, rs, **to):
        return pltpu.make_async_remote_copy(
            src_ref=src, dst_ref=dst, send_sem=ss, recv_sem=rs, device_id=to, device_id_type=MESH
        )

    for d in range(1, Z):
        to = (z + d) % Z
        remote(
            ld_hbm.at[:, pl.ds(to * L, L)], ldb.at[z], ld_s.at[d], ld_r.at[z], sp=to * X + x
        ).start()
    pltpu.make_async_copy(ld_hbm.at[:, pl.ds(z * L, L)], ldb.at[z], ld_r.at[z]).start()

    def send_rows(n, hbm, dst, ss, rs):
        s, j = n % G, n // G
        for d in (2, 1, 3) if X == 4 else range(1, X):
            to = (x + d) % X
            remote(hbm.at[s, to + X * j], dst, ss, rs, sp=z * X + to).start()
        pltpu.make_async_copy(hbm.at[s, x + X * j], dst, rs).start()

    @pl.loop(0, N)
    def _(n):
        mine = pl.ds(x * T, T)
        send_rows(n, k_hbm, kv.at[n, 0, mine], kv_s.at[n], kv_r.at[n])
        send_rows(n, v_hbm, kv.at[n, 1, mine], kv_s.at[n], kv_r.at[n])

    def ring_piece(k, sign):
        if k < R - 1:
            return pl.ds(0, HD)
        return pl.ds(0, HALF) if sign > 0 else pl.ds(HALF, HALF)

    def ring_send(k, sign):
        shard = dp_of(y - sign * k)
        rows = ring_piece(k, sign)
        src = w_hbm.at[rows] if k == 0 else wb.at[shard, rows]
        ss, rs = (wr_s, wr_r) if sign > 0 else (wl_s, wl_r)
        return remote(
            src, wb.at[shard, rows], ss.at[k], rs.at[k], dp=right if sign > 0 else left
        )

    def ring_recv(k, sign):
        shard = dp_of(y - sign * (k + 1))
        rs = wr_r if sign > 0 else wl_r
        take(wb.at[shard, ring_piece(k, sign)], rs.at[k])

    def to_mate(yy):
        shard = dp_of(yy)
        return remote(wb.at[shard], wb.at[shard], p_s.at[shard // 2], p_r.at[shard // 2], dp=mate)

    for sign in (1, -1):
        ring_send(0, sign).start()
    own_w = pltpu.make_async_copy(w_hbm, wb.at[dp], loc_w)
    own_w.start()
    remote(w_hbm, wb.at[dp], p_s.at[y], p_r.at[y], dp=mate).start()

    @pl.loop(0, N)
    def _(n):
        send_rows(n, q_hbm, qb.at[n, pl.ds(x * T, T)], q_s.at[n], q_r.at[n])

    @pl.when(z == 0)
    def _():
        s_in[...] = jnp.zeros_like(s_in)

    pos = (lax.broadcasted_iota(jnp.int32, (L, LANES), 0) + z * L).astype(F32)
    angle = pos * freq_ref[0:1, :]
    cosb[...] = jnp.cos(angle)
    sinb[...] = jnp.sin(angle)

    for i in range(Z):
        take(ldb.at[i], ld_r.at[i])
    run = jnp.concatenate([ldb[i] for i in range(Z)], axis=0)
    lane = lax.broadcasted_iota(jnp.int32, (Z, L), 1)
    step = 1
    while step < L:
        run = run + jnp.where(lane >= step, pltpu.roll(run, step, 1), 0.0)
        step *= 2
    cols = jnp.transpose(run)
    for i in range(Z):
        wrow[i] = run[i : i + 1]
        wcol[i] = jnp.broadcast_to(cols[:, i : i + 1], (L, LANES))

    def decay_row(n):
        return J * (n % G) + n // G

    def rotate(block):
        a, b = block[:, :LANES].astype(F32), block[:, LANES:].astype(F32)
        co, si = cosb[...], sinb[...]
        return (a * co - b * si).astype(BF16), (b * co + a * si).astype(BF16)

    def keys_in(n):
        i = decay_row(n)
        take(kv.at[n], kv_r.at[n])
        a, b = rotate(kv[n, 0])
        kv[n, 0, :, :LANES] = a
        kv[n, 0, :, LANES:] = b
        scale = jnp.exp(wcol[i, L - 1 : L, :] - wcol[i])
        scaled = jnp.concatenate(
            [(a.astype(F32) * scale).astype(BF16), (b.astype(F32) * scale).astype(BF16)], axis=1
        )
        got = lax.dot_general(
            scaled, kv[n, 1], (((0,), (0,)), ((), ())), preferred_element_type=F32
        )
        upd[n, 0] = got[:, :LANES]
        upd[n, 1] = got[:, LANES:]

    def chain_copy(n, hf):
        return remote(
            s_out.at[n, hf], s_in.at[n, hf], ch_s.at[n, hf], ch_r.at[n, hf],
            sp=jnp.minimum(z + 1, Z - 1) * X + x,
        )

    def chain(n):
        i = decay_row(n)
        factor = jnp.exp(wcol[i, L - 1 : L, :])
        for hf in range(2):
            @pl.when(z > 0)
            def _():
                take(s_in.at[n, hf], ch_r.at[n, hf])

            @pl.when(z < Z - 1)
            def _():
                s_out[n, hf] = (factor * s_in[n, hf].astype(F32) + upd[n, hf]).astype(BF16)
                chain_copy(n, hf).start()

    def outputs(n):
        i = decay_row(n)
        s, j = n % G, n // G
        take(qb.at[n], q_r.at[n])
        query = jnp.concatenate(rotate(qb[n]), axis=1)
        key, val = kv[n, 0], kv[n, 1]
        scores = lax.dot_general(
            query, key, (((1,), (1,)), ((), ())), preferred_element_type=F32
        )
        parts = []
        for m in range(L // LANES):
            lanes = slice(m * LANES, (m + 1) * LANES)
            spread = wcol[i] - wrow[i, :, lanes]
            causal = (
                lax.broadcasted_iota(jnp.int32, (L, LANES), 0)
                >= lax.broadcasted_iota(jnp.int32, (L, LANES), 1) + m * LANES
            )
            mask = jnp.where(causal, jnp.exp(jnp.where(causal, spread, 0.0)), 0.0)
            parts.append((scores[:, lanes] * mask).astype(BF16))
        weights = jnp.concatenate(parts, axis=1)
        local = jnp.dot(weights, val, preferred_element_type=F32)
        grow = jnp.exp(wcol[i])
        state = jnp.concatenate([s_in[n, 0], s_in[n, 1]], axis=1)
        carried = jnp.dot(query, state, preferred_element_type=F32)
        both = []
        for hf in range(2):
            lanes = slice(hf * LANES, (hf + 1) * LANES)
            both.append((local[:, lanes] + grow * carried[:, lanes]).astype(BF16).astype(F32))
        square = jnp.sum(both[0] * both[0] + both[1] * both[1], axis=1, keepdims=True)
        inv = lax.rsqrt(square * (1.0 / D) + 1e-6)
        o_snd[n, :, :LANES] = (both[0] * inv).astype(BF16)
        o_snd[n, :, LANES:] = (both[1] * inv).astype(BF16)
        rows = pl.ds(s * T, T)
        for d in (2, 1, 3) if X == 4 else range(1, X):
            to = (x + d) % X
            remote(
                o_snd.at[n, pl.ds(to * T, T)], o_rcv.at[j, x, rows], o_s.at[n], o_r.at[j, x],
                sp=z * X + to,
            ).start()
        o_rcv[j, x, rows, :] = o_snd[n, pl.ds(x * T, T), :]

    def ring_step(k):
        for sign in (1, -1):
            ring_recv(k - 1, sign)
            if k < R:
                ring_send(k, sign).start()
        if k < R:
            to_mate(y - k).start()
            to_mate(y + k).start()
        else:
            to_mate(y + R).start()

    lag = Z - 1 - z
    due = {k: jnp.maximum(4 * k + k // 3 - (6 * z + 4) // 5, 0) for k in range(1, R)}

    @pl.loop(0, N + Z - 1)
    def _(t):
        for k in range(1, R):
            @pl.when(t == due[k])
            def _(k=k):
                ring_step(k)

        @pl.when(t < N)
        def _():
            n = jnp.minimum(t, N - 1)
            keys_in(n)
            chain(n)

        @pl.when((t >= lag) & (t < lag + N))
        def _():
            outputs(jnp.clip(t - lag, 0, N - 1))

    ring_step(R)
    own_w.wait()
    for yy in range(Y):
        take(wb.at[2 * yy], p_r.at[yy])

    def project(j, yy):
        total = None
        for h in range(X):
            rows = slice((h + X * j) * D, (h + X * j + 1) * D)
            w_pair = jnp.concatenate([wb[2 * yy, rows, :], wb[2 * yy + 1, rows, :]], axis=1)
            term = jnp.dot(o_rcv[j, h], w_pair, preferred_element_type=F32)
            total = term if total is None else total + term
        return total

    for j in range(J):
        for d in range(1, X):
            src = (x + d) % X
            take(o_rcv.at[j, src], o_r.at[j, src])

        @pl.loop(0, Y)
        def _(yy):
            total = project(j, yy)
            if j > 0:
                total = total + acc[yy]
            if j < J - 1:
                acc[yy] = total
            else:
                cols2 = pl.ds(pl.multiple_of(yy * 2 * LANES, 2 * LANES), 2 * LANES)
                out_ref[:, cols2] = total.astype(BF16)

    for d in range(1, Z):
        take(ldb.at[0], ld_s.at[d])

    @pl.loop(0, N)
    def _(n):
        gone = pl.ds(0, (X - 1) * T)
        take(kv.at[n, :, gone], kv_s.at[n])
        take(qb.at[n, gone], q_s.at[n])
        take(qb.at[n, gone], o_s.at[n])

        @pl.when(z < Z - 1)
        def _():
            for hf in range(2):
                take(s_out.at[n, hf], ch_s.at[n, hf])

    for k in range(R):
        take(wb.at[0, ring_piece(k, 1)], wr_s.at[k])
        take(wb.at[0, ring_piece(k, -1)], wl_s.at[k])
    for yy in range(Y):
        take(wb.at[0], p_s.at[yy])


def on_device(queries, keys, values, log_decay, w_out):
    G, H, T, D = queries.shape
    X = RING_X
    Z = lax.axis_size("sp") // X
    Y = lax.axis_size("dp") // 2
    J = H // X
    N, L, HD = G * J, X * T, H * D
    F = w_out.shape[2]
    W = F * 2 * Y
    R = Y // 2
    assert N == Z and D == 2 * LANES and F == LANES and L == 2 * LANES
    half = D // 2
    freq = jnp.asarray(
        np.power(10000.0, -np.arange(half, dtype=np.float64) / half).astype(np.float32)
    ).reshape(1, half)
    dma = pltpu.SemaphoreType.DMA
    anyspace = pl.BlockSpec(memory_space=pl.ANY)
    vmem = pl.BlockSpec(memory_space=pltpu.VMEM)
    out = pl.pallas_call(
        functools.partial(kernel, (X, Z, Y, G, J, T, D)),
        out_shape=jax.ShapeDtypeStruct((G * T, W), BF16),
        in_specs=[anyspace] * 5 + [vmem],
        out_specs=vmem,
        scratch_shapes=[
            pltpu.VMEM((N, 2, L, D), BF16),
            pltpu.VMEM((N, L, D), BF16),
            pltpu.VMEM((Z, 1, L), F32),
            pltpu.VMEM((L, LANES), F32),
            pltpu.VMEM((L, LANES), F32),
            pltpu.VMEM((Z, 1, L), F32),
            pltpu.VMEM((Z, L, LANES), F32),
            pltpu.VMEM((N, 2, D, LANES), F32),
            pltpu.VMEM((N, 2, D, LANES), BF16),
            pltpu.VMEM((N, 2, D, LANES), BF16),
            pltpu.VMEM((N, L, D), BF16),
            pltpu.VMEM((J, X, G * T, D), BF16),
            pltpu.VMEM((2 * Y, HD, F), BF16),
            pltpu.VMEM((Y, G * T, 2 * F), F32),
            dma,
            dma((Z,)), dma((Z,)),
            dma((N,)), dma((N,)),
            dma((N,)), dma((N,)),
            dma((N, 2)), dma((N, 2)),
            dma((N,)), dma((J, X)),
            dma((R,)), dma((R,)), dma((R,)), dma((R,)),
            dma((Y,)), dma((Y,)),
        ],
        compiler_params=pltpu.CompilerParams(
            collective_id=0, has_side_effects=True, vmem_limit_bytes=48 * 1024 * 1024
        ),
        name="retention",
    )(queries, keys, values, log_decay, w_out.reshape(HD, F), freq)
    return out.reshape(G, T, W)


def solution(mesh):
    placed = (
        P("dp", None, "sp", None),
        P("dp", None, "sp", None),
        P("dp", None, "sp", None),
        P(("dp", "sp"), None),
        P(None, None, "dp"),
    )
    return jax.shard_map(
        on_device, mesh=mesh, in_specs=placed, out_specs=P("dp", "sp", None), check_vma=False
    )
```

```python
import functools

import jax
import jax.numpy as jnp
import numpy as np
from jax import lax
from jax.experimental import pallas as pl
from jax.experimental.pallas import tpu as pltpu
from jax.sharding import PartitionSpec as P

RING_X = 4
PIECES = 4
LANES = 128
MESH = pl.DeviceIdType.MESH
F32 = jnp.float32
BF16 = jnp.bfloat16


def take(ref, sem):
    pltpu.make_async_copy(ref, ref, sem).wait()


def kernel(
    dims,
    q_hbm, k_hbm, v_hbm, ld_hbm, w_hbm, freq_hbm,
    out_ref,
    kv, qb, ldb, cosb, sinb, wrow, wcol, upd, s_in, s_out, loc, o_snd, o_rcv, wb, acc, freq_ref,
    loc_f, loc_w, loc_d, loc_x, dr_s, dr_r, kv_s, kv_r, q_s, q_r, ch_s, ch_r, o_s, o_r,
    wr_s, wr_r, wl_s, wl_r, p_s, p_r,
):
    X, Z, Y, G, J, T, D = dims
    N, L, HD = G * J, X * T, X * J * D
    R = Y // 2
    HALF = HD // 2
    ROWS = D // PIECES
    sp, dp = lax.axis_index("sp"), lax.axis_index("dp")
    z, x = sp // X, sp % X
    y, c = dp // 2, dp % 2

    def dp_of(yy):
        return ((yy + 2 * Y) % Y) * 2 + c

    def sp_of(zz):
        return ((zz + Z) % Z) * X + x

    right, left, mate = dp_of(y + 1), dp_of(y - 1), y * 2 + (1 - c)
    up, down = sp_of(z + 1), sp_of(z - 1)
    partners = [{"sp": z * X + (x + d) % X} for d in range(1, X)] + [{"dp": right}, {"dp": left}]
    others = [{"sp": sp_of(z + d)} for d in range(1, Z)] + [{"dp": mate}]

    def remote(src, dst, ss, rs, **to):
        return pltpu.make_async_remote_copy(
            src_ref=src, dst_ref=dst, send_sem=ss, recv_sem=rs, device_id=to, device_id_type=MESH
        )

    freq_in = pltpu.make_async_copy(freq_hbm, freq_ref, loc_f)
    freq_in.start()
    own_w = pltpu.make_async_copy(w_hbm, wb.at[dp], loc_w)
    own_w.start()
    own_d = pltpu.make_async_copy(ld_hbm, ldb.at[z], loc_d)
    own_d.start()

    barrier = pltpu.get_barrier_semaphore()
    for to in partners + others:
        pl.semaphore_signal(barrier, inc=1, device_id=to, device_id_type=MESH)
    pl.semaphore_wait(barrier, len(partners) + len(others))

    def half(k, sign):
        first = (k % 2 == 0) == (sign > 0)
        return pl.ds(0, HALF) if first else pl.ds(HALF, HALF)

    def ring_send(k, sign):
        shard = dp_of(y - sign * (k // 2))
        rows = half(k, sign)
        src = w_hbm.at[rows] if k < 2 else wb.at[shard, rows]
        ss, rs = (wr_s, wr_r) if sign > 0 else (wl_s, wl_r)
        return remote(
            src, wb.at[shard, rows], ss.at[k], rs.at[k], dp=right if sign > 0 else left
        )

    def ring_step(k):
        for sign in (1, -1):
            shard = dp_of(y - sign * (k // 2 + 1))
            rows = half(k, sign)
            take(wb.at[shard, rows], (wr_r if sign > 0 else wl_r).at[k])
            if k + 2 < 2 * R - 1:
                ring_send(k + 2, sign).start()
            remote(
                wb.at[shard, rows], wb.at[shard, rows], p_s.at[shard // 2], p_r.at[shard // 2], dp=mate
            ).start()

    for k in range(min(2, 2 * R - 1)):
        for sign in (1, -1):
            ring_send(k, sign).start()

    mine = pl.ds(x * T, T)
    targets = [(x + d) % X for d in ((2, 1, 3) if X == 4 else range(1, X))]
    for n in range(N):
        heads, g = X * (n // G), n % G
        for m, hbm in enumerate((k_hbm, v_hbm)):
            for to in targets:
                remote(
                    hbm.at[g, to + heads], kv.at[n, m, mine], kv_s.at[n], kv_r.at[n], sp=z * X + to
                ).start()
    stay = []
    for j in range(J):
        items = pl.ds(j * G, G)
        for m, hbm in enumerate((k_hbm, v_hbm, q_hbm)):
            dst = qb.at[items, mine] if m == 2 else kv.at[items, m, mine]
            stay.append(pltpu.make_async_copy(hbm.at[:, x + X * j], dst, loc_x.at[j, m]))
            stay[-1].start()


    for d in range(1, Z):
        to = (z + d) % Z
        remote(ld_hbm, ldb.at[z], dr_s.at[d], dr_r.at[z], sp=to * X + x).start()
    remote(w_hbm, wb.at[dp], p_s.at[y], p_r.at[y], dp=mate).start()

    for j in range(J):
        for to in targets:
            remote(
                q_hbm.at[:, to + X * j], qb.at[pl.ds(j * G, G), mine], q_s.at[j], q_r.at[j],
                sp=z * X + to,
            ).start()

    @pl.when(z == 0)
    def _():
        s_in[...] = jnp.zeros_like(s_in)

    pos = (lax.broadcasted_iota(jnp.int32, (L, LANES), 0) + z * L).astype(F32)
    freq_in.wait()
    angle = pos * freq_ref[0:1, :]
    cosb[...] = jnp.cos(angle)
    sinb[...] = jnp.sin(angle)

    for d in range(1, Z):
        take(ldb.at[(z + d) % Z], dr_r.at[(z + d) % Z])
    own_d.wait()
    for copy in stay:
        copy.wait()

    here = pl.ds(pl.multiple_of(z * L, L), L)
    run = jnp.concatenate([ldb[i, :, here] for i in range(Z)], axis=0)
    lane = lax.broadcasted_iota(jnp.int32, (Z, L), 1)
    step = 1
    while step < L:
        run = run + jnp.where(lane >= step, pltpu.roll(run, step, 1), 0.0)
        step *= 2
    cols = jnp.transpose(run)
    for i in range(Z):
        wrow[i] = run[i : i + 1]
        wcol[i] = jnp.broadcast_to(cols[:, i : i + 1], (L, LANES))

    def decay_row(n):
        return J * (n % G) + n // G

    def rotate(block):
        a, b = block[:, :LANES].astype(F32), block[:, LANES:].astype(F32)
        co, si = cosb[...], sinb[...]
        return (a * co - b * si).astype(BF16), (b * co + a * si).astype(BF16)

    def keys_in(n):
        i = decay_row(n)
        take(kv.at[n, :, pl.ds(0, (X - 1) * T)], kv_r.at[n])
        a, b = rotate(kv[n, 0])
        kv[n, 0, :, :LANES] = a
        kv[n, 0, :, LANES:] = b
        scale = jnp.exp(wcol[i, L - 1 : L, :] - wcol[i])
        scaled = jnp.concatenate(
            [(a.astype(F32) * scale).astype(BF16), (b.astype(F32) * scale).astype(BF16)], axis=1
        )
        upd[n] = lax.dot_general(
            scaled, kv[n, 1], (((0,), (0,)), ((), ())), preferred_element_type=F32
        )

    def chain(n):
        factor = jnp.exp(wcol[decay_row(n), L - 1 : L, :])
        factor = jnp.concatenate([factor, factor], axis=1)
        for p in range(PIECES):
            rows = pl.ds(p * ROWS, ROWS)

            @pl.when(z > 0)
            def _():
                take(s_in.at[n, rows], ch_r.at[n, p])

            @pl.when(z < Z - 1)
            def _():
                s_out[n, rows, :] = (
                    factor * s_in[n, rows, :].astype(F32) + upd[n, rows, :]
                ).astype(BF16)
                remote(
                    s_out.at[n, rows], s_in.at[n, rows], ch_s.at[n, p], ch_r.at[n, p], sp=up
                ).start()

    def outputs_local(n):
        i = decay_row(n)

        @pl.when(n % G == 0)
        def _():
            take(qb.at[pl.ds(0, G), pl.ds(0, (X - 1) * T)], q_r.at[n // G])

        a, b = rotate(qb[n])
        qb[n, :, :LANES] = a
        qb[n, :, LANES:] = b
        scores = lax.dot_general(
            jnp.concatenate([a, b], axis=1), kv[n, 0], (((1,), (1,)), ((), ())),
            preferred_element_type=F32,
        )
        parts = []
        for m in range(L // LANES):
            lanes = slice(m * LANES, (m + 1) * LANES)
            spread = wcol[i] - wrow[i, :, lanes]
            causal = (
                lax.broadcasted_iota(jnp.int32, (L, LANES), 0)
                >= lax.broadcasted_iota(jnp.int32, (L, LANES), 1) + m * LANES
            )
            mask = jnp.where(causal, jnp.exp(jnp.where(causal, spread, 0.0)), 0.0)
            parts.append((scores[:, lanes] * mask).astype(BF16))
        weights = jnp.concatenate(parts, axis=1)
        loc[...] = jnp.dot(weights, kv[n, 1], preferred_element_type=F32)

    def outputs(n):
        s, j = n % G, n // G
        grow = jnp.exp(wcol[decay_row(n)])
        carried = jnp.dot(qb[n], s_in[n], preferred_element_type=F32)
        both = []
        for hf in range(2):
            lanes = slice(hf * LANES, (hf + 1) * LANES)
            both.append((loc[:, lanes] + grow * carried[:, lanes]).astype(BF16).astype(F32))
        square = jnp.sum(both[0] * both[0] + both[1] * both[1], axis=1, keepdims=True)
        inv = lax.rsqrt(square * (1.0 / D) + 1e-6)
        o_snd[n, :, :LANES] = (both[0] * inv).astype(BF16)
        o_snd[n, :, LANES:] = (both[1] * inv).astype(BF16)
        rows = pl.ds(s * T, T)
        for to in targets:
            remote(
                o_snd.at[n, pl.ds(to * T, T)], o_rcv.at[j, x, rows], o_s.at[n], o_r.at[j, x],
                sp=z * X + to,
            ).start()
        o_rcv[j, x, rows, :] = o_snd[n, pl.ds(x * T, T), :]

    lag = jnp.minimum(2 * (Z - 1 - z), N)
    last = N + Z

    def due(k):
        at = 18 + 20 * k - 9 * z
        late = 8 + jnp.maximum(at - 80, 0) // 5
        return jnp.clip(jnp.where(at > 80, late, at // 10), 0, last)

    @pl.loop(0, last + 1)
    def _(t):
        for k in range(2 * R - 1):
            @pl.when(t == due(k))
            def _(k=k):
                ring_step(k)

        n = jnp.clip(t - lag, 0, N - 1)
        leaving = (t >= lag) & (t < lag + N)

        @pl.when(t < N)
        def _():
            keys_in(jnp.minimum(t, N - 1))

        @pl.when(leaving)
        def _():
            outputs_local(n)

        @pl.when(t < N)
        def _():
            chain(jnp.minimum(t, N - 1))

        @pl.when(leaving)
        def _():
            outputs(n)

    own_w.wait()

    def project(j, yy):
        total = None
        for h in range(X):
            rows = slice((h + X * j) * D, (h + X * j + 1) * D)
            w_pair = jnp.concatenate([wb[2 * yy, rows, :], wb[2 * yy + 1, rows, :]], axis=1)
            term = jnp.dot(o_rcv[j, h], w_pair, preferred_element_type=F32)
            total = term if total is None else total + term
        return total

    for j in range(J):
        for d in range(1, X):
            src = (x + d) % X
            take(o_rcv.at[j, src], o_r.at[j, src])

        @pl.loop(0, Y)
        def _(k):
            yy = (y + Y + (1 - 2 * ((k + 1) % 2)) * ((k + 1) // 2)) % Y
            if j == 0:
                take(wb.at[0], p_r.at[yy])
            total = project(j, yy)
            if j > 0:
                total = total + acc[yy]
            if j < J - 1:
                acc[yy] = total
            else:
                cols2 = pl.ds(pl.multiple_of(yy * 2 * LANES, 2 * LANES), 2 * LANES)
                out_ref[:, cols2] = total.astype(BF16)

    for j in range(J):
        take(qb.at[pl.ds(0, G), pl.ds(0, (X - 1) * T)], q_s.at[j])
    for d in range(1, Z):
        take(ldb.at[0], dr_s.at[d])

    @pl.loop(0, N)
    def _(n):
        gone = pl.ds(0, (X - 1) * T)
        take(kv.at[n, :, gone], kv_s.at[n])
        take(qb.at[n, gone], o_s.at[n])

        @pl.when(z < Z - 1)
        def _():
            for p in range(PIECES):
                take(s_out.at[n, pl.ds(0, ROWS)], ch_s.at[n, p])

    for k in range(2 * R - 1):
        take(wb.at[0, pl.ds(0, HALF)], wr_s.at[k])
        take(wb.at[0, pl.ds(0, HALF)], wl_s.at[k])
    for yy in range(Y):
        take(wb.at[0], p_s.at[yy])


def on_device(queries, keys, values, log_decay, w_out):
    G, H, T, D = queries.shape
    X = RING_X
    Z = lax.axis_size("sp") // X
    Y = lax.axis_size("dp") // 2
    J = H // X
    N, L, HD = G * J, X * T, H * D
    F = w_out.shape[2]
    W = F * 2 * Y
    R = Y // 2
    assert N == Z and D == 2 * LANES and F == LANES and L == 2 * LANES
    half = D // 2
    freq = jnp.asarray(
        np.power(10000.0, -np.arange(half, dtype=np.float64) / half).astype(np.float32)
    ).reshape(1, half)
    dma = pltpu.SemaphoreType.DMA
    hbm = pl.BlockSpec(memory_space=pltpu.HBM)
    vmem = pl.BlockSpec(memory_space=pltpu.VMEM)
    out = pl.pallas_call(
        functools.partial(kernel, (X, Z, Y, G, J, T, D)),
        out_shape=jax.ShapeDtypeStruct((G * T, W), BF16),
        in_specs=[hbm] * 6,
        out_specs=vmem,
        scratch_shapes=[
            pltpu.VMEM((N, 2, L, D), BF16),
            pltpu.VMEM((N, L, D), BF16),
            pltpu.VMEM((Z, 1, Z * L), F32),
            pltpu.VMEM((L, LANES), F32),
            pltpu.VMEM((L, LANES), F32),
            pltpu.VMEM((Z, 1, L), F32),
            pltpu.VMEM((Z, L, LANES), F32),
            pltpu.VMEM((N, D, D), F32),
            pltpu.VMEM((N, D, D), BF16),
            pltpu.VMEM((N, D, D), BF16),
            pltpu.VMEM((L, D), F32),
            pltpu.VMEM((N, L, D), BF16),
            pltpu.VMEM((J, X, G * T, D), BF16),
            pltpu.VMEM((2 * Y, HD, F), BF16),
            pltpu.VMEM((Y, G * T, 2 * F), F32),
            pltpu.VMEM((1, LANES), F32),
            dma,
            dma,
            dma,
            dma((J, 3)),
            dma((Z,)), dma((Z,)),
            dma((N,)), dma((N,)),
            dma((J,)), dma((J,)),
            dma((N, PIECES)), dma((N, PIECES)),
            dma((N,)), dma((J, X)),
            dma((2 * R,)), dma((2 * R,)), dma((2 * R,)), dma((2 * R,)),
            dma((Y,)), dma((Y,)),
        ],
        compiler_params=pltpu.CompilerParams(
            collective_id=0, has_side_effects=True, vmem_limit_bytes=67043328
        ),
        name="retention",
    )(queries, keys, values, log_decay, w_out.reshape(HD, F), freq)
    return out.reshape(G, T, W)


def solution(mesh):
    placed = (
        P("dp", None, "sp", None),
        P("dp", None, "sp", None),
        P("dp", None, "sp", None),
        P(("dp", "sp"), None),
        P(None, None, "dp"),
    )
    return jax.shard_map(
        on_device, mesh=mesh, in_specs=placed, out_specs=P("dp", "sp", None), check_vma=False
    )
```

```python
import functools

import jax
import jax.numpy as jnp
import numpy as np
from jax import lax
from jax.experimental import pallas as pl
from jax.experimental.pallas import tpu as pltpu
from jax.sharding import PartitionSpec as P

RING_X = 4
PIECES = 4
LANES = 128
MESH = pl.DeviceIdType.MESH
F32 = jnp.float32
BF16 = jnp.bfloat16


def take(ref, sem):
    pltpu.make_async_copy(ref, ref, sem).wait()


def kernel(
    dims,
    q_hbm, k_hbm, v_hbm, ld_hbm, w_hbm, freq_hbm,
    out_ref,
    kv, qb, own_row, ldb, cosb, sinb, wrow, wcol, upd, s_in, s_out, loc, o_snd, o_rcv, wb, acc, freq_ref,
    loc_f, loc_w, loc_d, loc_x, dr_s, dr_r, kv_s, kv_r, q_s, q_r, ch_s, ch_r, o_s, o_r,
    wr_s, wr_r, wl_s, wl_r, p_s, p_r,
):
    X, Z, Y, G, J, T, D = dims
    N, L, HD = G * J, X * T, X * J * D
    R = Y // 2
    HALF = HD // 2
    ROWS = D // PIECES
    sp, dp = lax.axis_index("sp"), lax.axis_index("dp")
    z, x = sp // X, sp % X
    y, c = dp // 2, dp % 2

    def dp_of(yy):
        return ((yy + 2 * Y) % Y) * 2 + c

    def sp_of(zz):
        return ((zz + Z) % Z) * X + x

    right, left, mate = dp_of(y + 1), dp_of(y - 1), y * 2 + (1 - c)
    up, down = sp_of(z + 1), sp_of(z - 1)
    partners = [{"sp": z * X + (x + d) % X} for d in range(1, X)] + [{"dp": right}, {"dp": left}, {"dp": mate}]

    def remote(src, dst, ss, rs, **to):
        return pltpu.make_async_remote_copy(
            src_ref=src, dst_ref=dst, send_sem=ss, recv_sem=rs, device_id=to, device_id_type=MESH
        )

    freq_in = pltpu.make_async_copy(freq_hbm, freq_ref, loc_f)
    freq_in.start()
    own_w = pltpu.make_async_copy(w_hbm, wb.at[dp], loc_w)
    own_w.start()
    own_d = pltpu.make_async_copy(ld_hbm, own_row, loc_d)
    own_d.start()

    barrier = pltpu.get_barrier_semaphore()
    for to in partners:
        pl.semaphore_signal(barrier, inc=1, device_id=to, device_id_type=MESH)
    for d in range(1, Z):

        @pl.when((z + d) % Z != 0)
        def _():
            pl.semaphore_signal(barrier, inc=1, device_id={"sp": sp_of(z + d)}, device_id_type=MESH)

    pl.semaphore_wait(barrier, len(partners) + jnp.where(z == 0, 0, Z - 1))

    def half(k, sign):
        first = (k % 2 == 0) == (sign > 0)
        return pl.ds(0, HALF) if first else pl.ds(HALF, HALF)

    def ring_send(k, sign):
        shard = dp_of(y - sign * (k // 2))
        rows = half(k, sign)
        src = w_hbm.at[rows] if k < 2 else wb.at[shard, rows]
        ss, rs = (wr_s, wr_r) if sign > 0 else (wl_s, wl_r)
        return remote(
            src, wb.at[shard, rows], ss.at[k], rs.at[k], dp=right if sign > 0 else left
        )

    def ring_step(k):
        for sign in (1, -1):
            shard = dp_of(y - sign * (k // 2 + 1))
            rows = half(k, sign)
            take(wb.at[shard, rows], (wr_r if sign > 0 else wl_r).at[k])
            if k + 2 < 2 * R - 1:
                ring_send(k + 2, sign).start()
            remote(
                wb.at[shard, rows], wb.at[shard, rows], p_s.at[shard // 2], p_r.at[shard // 2], dp=mate
            ).start()

    def send_decays():
        for d in range(1, Z):
            to = (z + d) % Z
            remote(
                own_row.at[:, pl.ds(pl.multiple_of(to * L, L), L)], ldb.at[z], dr_s.at[d], dr_r.at[z],
                sp=to * X + x,
            ).start()

    own_d.wait()
    pl.when(z > 0)(send_decays)

    mine = pl.ds(x * T, T)
    targets = [(x + d) % X for d in ((2, 1, 3) if X == 4 else range(1, X))]

    def send_keys(n):
        heads, g = X * (J - 1 - n // G), n % G
        for m, hbm in enumerate((k_hbm, v_hbm)):
            for to in targets:
                remote(
                    hbm.at[g, to + heads], kv.at[n, m, mine], kv_s.at[n], kv_r.at[n], sp=z * X + to
                ).start()

    send_keys(0)
    for k in range(min(2, 2 * R - 1)):
        for sign in (1, -1):
            ring_send(k, sign).start()
    for n in range(1, N):
        send_keys(n)
    stay = []
    for j in range(J):
        items = pl.ds((J - 1 - j) * G, G)
        for m, hbm in enumerate((k_hbm, v_hbm, q_hbm)):
            dst = qb.at[items, mine] if m == 2 else kv.at[items, m, mine]
            stay.append(pltpu.make_async_copy(hbm.at[:, x + X * j], dst, loc_x.at[j, m]))
            stay[-1].start()

    remote(w_hbm, wb.at[dp], p_s.at[y], p_r.at[y], dp=mate).start()

    for j in range(J):
        for to in targets:
            remote(
                q_hbm.at[:, to + X * (J - 1 - j)], qb.at[pl.ds(j * G, G), mine], q_s.at[j], q_r.at[j],
                sp=z * X + to,
            ).start()

    @pl.when(z == 0)
    def _():
        s_in[...] = jnp.zeros_like(s_in)

    pos = (lax.broadcasted_iota(jnp.int32, (L, LANES), 0) + z * L).astype(F32)
    freq_in.wait()
    angle = pos * freq_ref[0:1, :]
    cosb[...] = jnp.cos(angle)
    sinb[...] = jnp.sin(angle)

    ldb[z] = own_row[:, pl.ds(pl.multiple_of(z * L, L), L)]

    def decays(rows):
        run = jnp.concatenate([ldb[rows[i % len(rows)]] for i in range(8)], axis=0)
        lane = lax.broadcasted_iota(jnp.int32, (8, L), 1)
        step = 1
        while step < L:
            run = run + jnp.where(lane >= step, pltpu.roll(run, step, 1), 0.0)
            step *= 2
        cols = jnp.transpose(run)
        for k, i in enumerate(rows):
            wrow[i] = run[k : k + 1]
            wcol[i] = jnp.broadcast_to(cols[:, k : k + 1], (L, LANES))

    def rows_in(rows):
        for i in rows:

            @pl.when(z != i)
            def _(i=i):
                take(ldb.at[i], dr_r.at[i])

    first = J - 1

    @pl.when(z == 0)
    def _():
        rows_in(range(1, Z))
        send_decays()

    @pl.when(z > 0)
    def _():
        rows_in([first] if first > 0 else [])

    decays([first])

    def middle_decays():
        rows = [i for i in range(1, Z) if i != first]
        pl.when(z > 0)(lambda: rows_in(rows))
        if rows:
            decays(rows)

    def last_decays():
        pl.when(z > 0)(lambda: rows_in([0]))
        decays([0])

    for copy in stay:
        copy.wait()

    def decay_row(n):
        return J * (n % G) + J - 1 - n // G

    def rotate(block):
        a, b = block[:, :LANES].astype(F32), block[:, LANES:].astype(F32)
        co, si = cosb[...], sinb[...]
        return (a * co - b * si).astype(BF16), (b * co + a * si).astype(BF16)

    def keys_in(n):
        i = decay_row(n)
        take(kv.at[n, :, pl.ds(0, (X - 1) * T)], kv_r.at[n])
        a, b = rotate(kv[n, 0])
        kv[n, 0, :, :LANES] = a
        kv[n, 0, :, LANES:] = b
        scale = jnp.exp(wcol[i, L - 1 : L, :] - wcol[i])
        scaled = jnp.concatenate(
            [(a.astype(F32) * scale).astype(BF16), (b.astype(F32) * scale).astype(BF16)], axis=1
        )
        upd[n] = lax.dot_general(
            scaled, kv[n, 1], (((0,), (0,)), ((), ())), preferred_element_type=F32
        )

    def chain(n):
        factor = jnp.exp(wcol[decay_row(n), L - 1 : L, :])
        factor = jnp.concatenate([factor, factor], axis=1)
        for p in range(PIECES):
            rows = pl.ds(p * ROWS, ROWS)

            @pl.when(z > 0)
            def _():
                take(s_in.at[n, rows], ch_r.at[n, p])

            @pl.when(z < Z - 1)
            def _():
                s_out[n, rows, :] = (
                    factor * s_in[n, rows, :].astype(F32) + upd[n, rows, :]
                ).astype(BF16)
                remote(
                    s_out.at[n, rows], s_in.at[n, rows], ch_s.at[n, p], ch_r.at[n, p], sp=up
                ).start()

    def outputs_local(n):
        i = decay_row(n)

        @pl.when(n % G == 0)
        def _():
            take(qb.at[pl.ds(0, G), pl.ds(0, (X - 1) * T)], q_r.at[n // G])

        a, b = rotate(qb[n])
        qb[n, :, :LANES] = a
        qb[n, :, LANES:] = b
        scores = lax.dot_general(
            jnp.concatenate([a, b], axis=1), kv[n, 0], (((1,), (1,)), ((), ())),
            preferred_element_type=F32,
        )
        parts = []
        for m in range(L // LANES):
            lanes = slice(m * LANES, (m + 1) * LANES)
            spread = wcol[i] - wrow[i, :, lanes]
            causal = (
                lax.broadcasted_iota(jnp.int32, (L, LANES), 0)
                >= lax.broadcasted_iota(jnp.int32, (L, LANES), 1) + m * LANES
            )
            mask = jnp.where(causal, jnp.exp(jnp.where(causal, spread, 0.0)), 0.0)
            parts.append((scores[:, lanes] * mask).astype(BF16))
        weights = jnp.concatenate(parts, axis=1)
        loc[...] = jnp.dot(weights, kv[n, 1], preferred_element_type=F32)

    def outputs(n):
        s, j = n % G, J - 1 - n // G
        grow = jnp.exp(wcol[decay_row(n)])
        carried = jnp.dot(qb[n], s_in[n], preferred_element_type=F32)
        both = []
        for hf in range(2):
            lanes = slice(hf * LANES, (hf + 1) * LANES)
            both.append((loc[:, lanes] + grow * carried[:, lanes]).astype(BF16).astype(F32))
        square = jnp.sum(both[0] * both[0] + both[1] * both[1], axis=1, keepdims=True)
        inv = lax.rsqrt(square * (1.0 / D) + 1e-6)
        o_snd[n, :, :LANES] = (both[0] * inv).astype(BF16)
        o_snd[n, :, LANES:] = (both[1] * inv).astype(BF16)
        rows = pl.ds(s * T, T)
        for to in targets:
            remote(
                o_snd.at[n, pl.ds(to * T, T)], o_rcv.at[j, x, rows], o_s.at[n], o_r.at[j, x],
                sp=z * X + to,
            ).start()
        o_rcv[j, x, rows, :] = o_snd[n, pl.ds(x * T, T), :]

    lag = jnp.where(z == Z - 1, 0, jnp.minimum(Z + 1 - z, N))
    last = N + Z

    def due(k):
        at = 18 + 20 * k - 9 * z
        late = 8 + jnp.maximum(at - 80, 0) // 5
        return jnp.clip(jnp.where(at > 80, late, at // 10), 0, last)

    @pl.loop(0, last + 1)
    def _(t):
        for k in range(2 * R - 1):
            @pl.when(t == due(k))
            def _(k=k):
                ring_step(k)

        if Z > 1:
            pl.when(t == 1)(middle_decays)
            pl.when(t == G)(last_decays)

        n = jnp.clip(t - lag, 0, N - 1)
        leaving = (t >= lag) & (t < lag + N)

        @pl.when(t < N)
        def _():
            keys_in(jnp.minimum(t, N - 1))

        @pl.when(leaving & (z == Z - 1))
        def _():
            outputs_local(n)

        @pl.when(t < N)
        def _():
            chain(jnp.minimum(t, N - 1))

        @pl.when(leaving & (z < Z - 1))
        def _():
            outputs_local(n)

        @pl.when(leaving)
        def _():
            outputs(n)

    own_w.wait()

    def project(j, yy):
        total = None
        for h in range(X):
            rows = slice((h + X * j) * D, (h + X * j + 1) * D)
            w_pair = jnp.concatenate([wb[2 * yy, rows, :], wb[2 * yy + 1, rows, :]], axis=1)
            term = jnp.dot(o_rcv[j, h], w_pair, preferred_element_type=F32)
            total = term if total is None else total + term
        return total

    for at, j in enumerate(reversed(range(J))):
        for d in range(1, X):
            src = (x + d) % X
            take(o_rcv.at[j, src], o_r.at[j, src])

        @pl.loop(0, Y)
        def _(k):
            yy = (y + Y + (1 - 2 * ((k + 1) % 2)) * ((k + 1) // 2)) % Y
            if at == 0:
                take(wb.at[0], p_r.at[yy])
            total = project(j, yy)
            if at > 0:
                total = total + acc[yy]
            if at < J - 1:
                acc[yy] = total
            else:
                cols2 = pl.ds(pl.multiple_of(yy * 2 * LANES, 2 * LANES), 2 * LANES)
                out_ref[:, cols2] = total.astype(BF16)

    for j in range(J):
        take(qb.at[pl.ds(0, G), pl.ds(0, (X - 1) * T)], q_s.at[j])
    for d in range(1, Z):
        take(ldb.at[0], dr_s.at[d])

    @pl.loop(0, N)
    def _(n):
        gone = pl.ds(0, (X - 1) * T)
        take(kv.at[n, :, gone], kv_s.at[n])
        take(qb.at[n, gone], o_s.at[n])

        @pl.when(z < Z - 1)
        def _():
            for p in range(PIECES):
                take(s_out.at[n, pl.ds(0, ROWS)], ch_s.at[n, p])

    for k in range(2 * R - 1):
        take(wb.at[0, pl.ds(0, HALF)], wr_s.at[k])
        take(wb.at[0, pl.ds(0, HALF)], wl_s.at[k])
    for yy in range(Y):
        take(wb.at[0], p_s.at[yy])


def on_device(queries, keys, values, log_decay, w_out):
    G, H, T, D = queries.shape
    X = RING_X
    Z = lax.axis_size("sp") // X
    Y = lax.axis_size("dp") // 2
    J = H // X
    N, L, HD = G * J, X * T, H * D
    F = w_out.shape[2]
    W = F * 2 * Y
    R = Y // 2
    assert N == Z and D == 2 * LANES and F == LANES and L == 2 * LANES
    half = D // 2
    freq = jnp.asarray(
        np.power(10000.0, -np.arange(half, dtype=np.float64) / half).astype(np.float32)
    ).reshape(1, half)
    dma = pltpu.SemaphoreType.DMA
    hbm = pl.BlockSpec(memory_space=pltpu.HBM)
    vmem = pl.BlockSpec(memory_space=pltpu.VMEM)
    out = pl.pallas_call(
        functools.partial(kernel, (X, Z, Y, G, J, T, D)),
        out_shape=jax.ShapeDtypeStruct((G * T, W), BF16),
        in_specs=[hbm] * 6,
        out_specs=vmem,
        scratch_shapes=[
            pltpu.VMEM((N, 2, L, D), BF16),
            pltpu.VMEM((N, L, D), BF16),
            pltpu.VMEM((1, Z * L), F32),
            pltpu.VMEM((Z, 1, L), F32),
            pltpu.VMEM((L, LANES), F32),
            pltpu.VMEM((L, LANES), F32),
            pltpu.VMEM((Z, 1, L), F32),
            pltpu.VMEM((Z, L, LANES), F32),
            pltpu.VMEM((N, D, D), F32),
            pltpu.VMEM((N, D, D), BF16),
            pltpu.VMEM((N, D, D), BF16),
            pltpu.VMEM((L, D), F32),
            pltpu.VMEM((N, L, D), BF16),
            pltpu.VMEM((J, X, G * T, D), BF16),
            pltpu.VMEM((2 * Y, HD, F), BF16),
            pltpu.VMEM((Y, G * T, 2 * F), F32),
            pltpu.VMEM((1, LANES), F32),
            dma,
            dma,
            dma,
            dma((J, 3)),
            dma((Z,)), dma((Z,)),
            dma((N,)), dma((N,)),
            dma((J,)), dma((J,)),
            dma((N, PIECES)), dma((N, PIECES)),
            dma((N,)), dma((J, X)),
            dma((2 * R,)), dma((2 * R,)), dma((2 * R,)), dma((2 * R,)),
            dma((Y,)), dma((Y,)),
        ],
        compiler_params=pltpu.CompilerParams(
            collective_id=0, has_side_effects=True, vmem_limit_bytes=67043328
        ),
        name="retention",
    )(queries, keys, values, log_decay, w_out.reshape(HD, F), freq)
    return out.reshape(G, T, W)


def solution(mesh):
    placed = (
        P("dp", None, "sp", None),
        P("dp", None, "sp", None),
        P("dp", None, "sp", None),
        P(("dp", "sp"), None),
        P(None, None, "dp"),
    )
    return jax.shard_map(
        on_device, mesh=mesh, in_specs=placed, out_specs=P("dp", "sp", None), check_vma=False
    )
```
